32 devices in a mesh: ep: 8 (over z, core), tp: 4 (over y, x).
Axes of the slice: x: 2, y: 2, z: 4, core: 2. Of those that a mesh axis runs over, the one named last changes fastest.
Arguments:
- mix_in: bfloat16 [1024, 2048], P('ep'), may hold values from -6 to 6
- mix_gain: float32 [2048], replicated, may hold values from 0.1 to 1.9
- lam_re: float32 [128, 64], P('tp'), may hold values from -0.34 to -1e-05
- lam_im: float32 [128, 64], P('tp'), may hold values from 0.2 to 4
- log_dt: float32 [128], P('tp'), may hold values from -2.31 to 0
- b_re: float32 [128, 64, 16], P('tp'), may hold values from -0.125 to 0.125
- b_im: float32 [128, 64, 16], P('tp'), may hold values from -0.125 to 0.125
- c_re: float32 [128, 16, 64], P('tp'), may hold values from -0.5 to 0.5
- c_im: float32 [128, 16, 64], P('tp'), may hold values from -0.5 to 0.5
- d_skip: float32 [2048], P('tp'), may hold values from -2 to 2
- log_retain: float32 [1024, 128], P('ep', 'tp'), may hold values from -2.2 to 0
- w_lin: bfloat16 [2048, 2048], P(None, 'tp'), may hold values from -0.125 to 0.125
- w_glu: bfloat16 [2048, 2048], P(None, 'tp'), may hold values from -0.125 to 0.125
- moe_in: bfloat16 [1024, 2048], P('ep'), may hold values from -6 to 6
- moe_gain: float32 [2048], replicated, may hold values from 0.1 to 1.9
- routes: int32 [1024, 2], P('ep'), may hold values from 0 to 7, all different within a row; in each aligned block of 128 rows (0 to 127, 128 to 255, ...) at most 48 rows name the same one
- route_weight: float32 [1024, 2], P('ep'), may hold values from 0.1 to 1
- w_gate: bfloat16 [8, 2048, 4096], P('ep', None, 'tp'), may hold values from -0.125 to 0.125
- w_up: bfloat16 [8, 2048, 4096], P('ep', None, 'tp'), may hold values from -0.125 to 0.125
- w_down: bfloat16 [8, 4096, 2048], P('ep', 'tp'), may hold values from -0.09375 to 0.09375
Outputs:
- mix_out: bfloat16 [1024, 2048], P('ep', 'tp')
- moe_out: bfloat16 [1024, 2048], P('ep', 'tp')
The draws below stay inside these ranges and needn't reach their ends.
Inputs may be any that keep to these rules, and one draw needn't show every extreme that they name: `routes`: each row names 2 different experts. In each aligned block of 128 rows (the rows of one index of ep) no expert is named by more than 48 rows, and in some block an expert is named by exactly 48 rows.
All inputs are finite; a program needn't handle non-finite values.
Results may differ from the reference program's by a relative error of at most 0.015.
Values may be sent and summed in bfloat16 or wider, within the bound.
A program may use at most 192 MiB of HBM per device.

```python
import math
import jax
import jax.numpy as jnp
import numpy as np
from jax import lax

D = 2048
GROUP_CH = 16
STATE = 64
H = 4096
TOP = 2
TA_DEV = 128
TB_DEV = 128
GROUPS = 128
EXPERTS = 8
CAP = 48
TOKA = 1024
TOKB = 1024
N_EP = 8
N_TP = 4


def shared_steps(key):
    step_key = jax.random.fold_in(key, 11)
    return jax.random.uniform(step_key, (GROUPS,), jnp.float32, math.log(0.1), 0.0)


def draw_log_dt(key, part):
    return shared_steps(key)


def draw_lam_re(key, part):
    time_step = jnp.exp(shared_steps(key))[:, None]
    slow_share = 0.5
    chooser = jax.random.uniform(jax.random.fold_in(key, 12), (GROUPS, STATE), jnp.float32)
    slow_rate = jnp.exp(jax.random.uniform(jax.random.fold_in(key, 13), (GROUPS, STATE), jnp.float32, math.log(1e-05), math.log(5e-05)))
    fast_rate = jnp.exp(jax.random.uniform(jax.random.fold_in(key, 14), (GROUPS, STATE), jnp.float32, math.log(0.01), math.log(0.033)))
    rate = jnp.where(chooser < slow_share, slow_rate, fast_rate)
    return -rate / time_step


def draw_log_retain(key, part):
    blocks = TOKA // TA_DEV
    steady_rate = jnp.exp(jax.random.uniform(jax.random.fold_in(key, 21), (blocks, 1, GROUPS), jnp.float32, math.log(0.3), math.log(1.2))) / TOKA
    stable_level = -jnp.broadcast_to(steady_rate, (blocks, TA_DEV, GROUPS)).reshape(TOKA, GROUPS)
    spots = jax.random.randint(jax.random.fold_in(key, 22), (3, GROUPS), 0, TOKA)
    loss_values = jnp.log(jax.random.uniform(jax.random.fold_in(key, 23), (3, GROUPS), jnp.float32, 0.5, 0.8))
    spot_matches = jnp.arange(TOKA, dtype=jnp.int32)[:, None, None] == spots[None]
    token_spurts = jnp.sum(jnp.where(spot_matches, loss_values[None], 0.0), axis=1)
    return stable_level + token_spurts


def block_scale(stream_key, extent, cuts, least, largest):
    loudness = 1.0
    for axis_at, blocks in cuts:
        heights = jax.random.uniform(jax.random.fold_in(jax.random.fold_in(stream_key, 6), axis_at), (blocks,), jnp.float32, least / len(cuts), largest / len(cuts))
        loudness = loudness * jnp.repeat(jnp.exp(heights), extent[axis_at] // blocks).reshape((-1,) + (1,) * (len(extent) - 1 - axis_at))
    return loudness


def assign_block(rng, own, number, rows, number_of, top, reach, lean):
    ranking = jax.random.permutation(rng, number_of)
    heavy_load, usual = shares(number_of, rows * top, reach, lean, True), shares(number_of, rows * top, reach, lean, False)
    places = jnp.arange(number_of)

    def named(tallies, offset_by):
        used = int((tallies > 0).sum())
        fixed = max(1, used // 4)
        moved = fixed + (places - fixed + offset_by * (used - fixed)) % max(1, number_of - fixed)
        return jnp.zeros((number_of,), jnp.int32).at[ranking[jnp.where(places < fixed, places, moved)]].set(jnp.asarray(tallies, jnp.int32))

    tallies = jnp.where(number % 4 == 0, named(heavy_load, number // 4), named(usual, number - number // 4 - 1))
    mixed = jax.random.permutation(jax.random.fold_in(own, 3), number_of)
    source_of, receiver = mixed[0:number_of // 2 * 2:2], mixed[1:number_of // 2 * 2:2]
    slack = jnp.minimum(tallies[source_of] - 1, reach - tallies[receiver]) // 2
    slack = jnp.where((source_of == ranking[0]) | (receiver == ranking[0]) | (tallies[receiver] == 0), 0, jnp.maximum(slack, 0))
    moved = jax.random.randint(jax.random.fold_in(own, 4), (number_of // 2,), 0, 1 << 20) % (slack + 1)
    tallies = tallies.at[source_of].add(-moved).at[receiver].add(moved)
    members = jnp.searchsorted(jnp.cumsum(tallies), jnp.arange(rows * top), side="right").astype(jnp.int32)
    listing = members.reshape(top, rows).T
    listing = listing[jax.random.permutation(jax.random.fold_in(own, 1), rows)]
    offset_by = jax.random.randint(jax.random.fold_in(own, 2), (rows, 1), 0, top)
    return jnp.take_along_axis(listing, (jnp.arange(top)[None, :] + offset_by) % top, axis=1)


def shares(count, total, bound, lean, full):
    weights = [(1 << 20) // math.isqrt(grade ** lean) + 1 for grade in range(1, count + 1)]
    largest = bound if full else min(bound, max(-(-total // count), total * weights[0] // sum(weights)))
    least = 1 if total - largest >= count - 1 else 0
    given, rest = [largest] + [least] * (count - 1), total - largest - least * (count - 1)
    while rest > 0:
        candidates = [i for i in range(1, count) if given[i] < largest] or [i for i in range(1, count) if given[i] < bound]
        pool, remaining = sum([weights[i] for i in candidates]), rest
        for i in candidates:
            extra = min(bound - given[i], max(1, remaining * weights[i] // pool), rest)
            given[i] = given[i] + extra
            rest = rest - extra
    return np.array(given)


def centred(rng, extent, width, limit, split=(), held_as=jnp.bfloat16):
    entries = jax.random.normal(rng, extent, jnp.float32) * width
    if len(split) > 0:
        entries = block_scale(rng, extent, split, -0.22, 0.18) * entries
    return jnp.clip(entries, min=-limit, max=limit).astype(held_as)


def setup_inputs(seed: int = 0) -> dict:
    streams_of = jax.random.split(jax.random.key(seed), 21)
    mix_in = centred(streams_of[0], (TOKA, D), 1.0, 6.0, ((0, 8),))
    mix_gain = jnp.clip(1.0 + 0.18 * jax.random.normal(streams_of[1], (D,), jnp.float32), 0.1, 1.9)
    lam_re = draw_lam_re(jax.random.fold_in(streams_of[20], 71), 0)
    lam_im = jnp.clip(0.2 + 3.8 * jax.random.uniform(streams_of[3], (GROUPS, STATE), jnp.float32) ** block_scale(streams_of[3], (GROUPS, STATE), ((0, 4),), -0.2, 0.2), 0.2, 4.0)
    log_dt = draw_log_dt(jax.random.fold_in(streams_of[20], 71), 0)
    b_re = centred(streams_of[5], (GROUPS, STATE, GROUP_CH), (GROUP_CH * TOKA // 8) ** -0.5, 0.125, ((0, 4),), jnp.float32)
    b_im = centred(streams_of[6], (GROUPS, STATE, GROUP_CH), (GROUP_CH * TOKA // 8) ** -0.5, 0.125, ((0, 4),), jnp.float32)
    c_re = centred(streams_of[7], (GROUPS, GROUP_CH, STATE), (2 * STATE) ** -0.5, 0.5, ((0, 4),), jnp.float32)
    c_im = centred(streams_of[8], (GROUPS, GROUP_CH, STATE), (2 * STATE) ** -0.5, 0.5, ((0, 4),), jnp.float32)
    d_skip = centred(streams_of[9], (D,), 0.5, 2.0, ((0, 4),), jnp.float32)
    log_retain = draw_log_retain(jax.random.fold_in(streams_of[20], 71), 0)
    w_lin = centred(streams_of[11], (D, D), D ** -0.5, 0.125, ((1, 4),))
    w_glu = centred(streams_of[12], (D, D), D ** -0.5, 0.125, ((1, 4),))
    moe_in = centred(streams_of[13], (TOKB, D), 1.0, 6.0, ((0, 8),))
    moe_gain = jnp.clip(1.0 + 0.18 * jax.random.normal(streams_of[14], (D,), jnp.float32), 0.1, 1.9)
    routes_keys = jax.random.split(jax.random.fold_in(streams_of[15], 1), TOKB // TB_DEV)
    routes_turns = jax.random.permutation(jax.random.fold_in(streams_of[15], 3), TOKB // TB_DEV)
    routes = jax.vmap(lambda own, number: assign_block(jax.random.fold_in(streams_of[15], 2), own, number, TB_DEV, EXPERTS, TOP, CAP, 2))(routes_keys, routes_turns).reshape((TOKB, TOP))
    route_weight = jnp.clip(jnp.exp(math.log(1.0) - 2.3025851 * jax.random.uniform(streams_of[16], (TOKB, TOP), jnp.float32) ** block_scale(streams_of[16], (TOKB, TOP), ((0, 8),), -0.2, 0.2)), 0.1, 1.0)
    w_gate = centred(streams_of[17], (EXPERTS, D, H), D ** -0.5, 0.125, ((0, 8), (2, 4)))
    w_up = centred(streams_of[18], (EXPERTS, D, H), D ** -0.5, 0.125, ((0, 8), (2, 4)))
    w_down = centred(streams_of[19], (EXPERTS, H, D), H ** -0.5, 0.09375, ((0, 8), (1, 4)))
    return {"mix_in": mix_in, "mix_gain": mix_gain, "lam_re": lam_re, "lam_im": lam_im, "log_dt": log_dt, "b_re": b_re, "b_im": b_im, "c_re": c_re, "c_im": c_im, "d_skip": d_skip, "log_retain": log_retain, "w_lin": w_lin, "w_glu": w_glu, "moe_in": moe_in, "moe_gain": moe_gain, "routes": routes, "route_weight": route_weight, "w_gate": w_gate, "w_up": w_up, "w_down": w_down}


EPS = 1e-06
HIGHEST = lax.Precision.HIGHEST

def root_mean_normed(values, gain):
    broadened_rows = values.astype(jnp.float32)
    inverse = lax.rsqrt(lax.optimization_barrier(jnp.mean(broadened_rows * broadened_rows, axis=-1, keepdims=True)) + EPS)
    return (broadened_rows * inverse * gain.astype(jnp.float32)).astype(jnp.bfloat16)

def compose(earlier, later):
    early_re, early_im, shift_re, shift_im = earlier
    late_re, late_im, offset_re, offset_im = later
    return (late_re * early_re - late_im * early_im, late_re * early_im + late_im * early_re, late_re * shift_re - late_im * shift_im + offset_re, late_re * shift_im + late_im * shift_re + offset_im)

def discretize(lam_re, lam_im, log_dt, b_re, b_im):
    time_step = jnp.exp(log_dt)[:, None]
    log_mag = lam_re * time_step
    angle = lam_im * time_step
    half_sine = jnp.sin(0.5 * angle)
    minus_re = jnp.expm1(log_mag) * jnp.cos(angle) - 2.0 * half_sine * half_sine
    minus_im = jnp.exp(log_mag) * jnp.sin(angle)
    denom = lam_re * lam_re + lam_im * lam_im
    coef_re = (minus_re * lam_re + minus_im * lam_im) / denom
    coef_im = (minus_im * lam_re - minus_re * lam_im) / denom
    drive_re = coef_re[..., None] * b_re - coef_im[..., None] * b_im
    drive_im = coef_re[..., None] * b_im + coef_im[..., None] * b_re
    return (log_mag, angle, drive_re, drive_im)

def local_scan(inputs, retain, log_mag, angle, drive_re, drive_im):
    length = inputs.shape[0]
    groups, states, channels = drive_re.shape
    broadened_rows = inputs.astype(jnp.float32).reshape(length, groups, channels)
    push_re = jnp.einsum('tgn,gpn->tgp', broadened_rows, drive_re, precision=HIGHEST).reshape(length, groups * states)
    push_im = jnp.einsum('tgn,gpn->tgp', broadened_rows, drive_im, precision=HIGHEST).reshape(length, groups * states)
    magnitude = jnp.exp(log_mag[None] + retain[:, :, None]).reshape(length, groups * states)
    decay_re = magnitude * jnp.cos(angle).reshape(1, groups * states)
    decay_im = magnitude * jnp.sin(angle).reshape(1, groups * states)
    return lax.associative_scan(compose, (decay_re, decay_im, push_re, push_im), axis=0)

def read_out(total_re, total_im, inputs, c_re, c_im, d_skip):
    length = inputs.shape[0]
    groups, channels, states = c_re.shape
    state_re = total_re.reshape(length, groups, states)
    state_im = total_im.reshape(length, groups, states)
    mixed = jnp.einsum('tgp,gnp->tgn', state_re, c_re, precision=HIGHEST)
    mixed = mixed - jnp.einsum('tgp,gnp->tgn', state_im, c_im, precision=HIGHEST)
    skipped = mixed.reshape(length, groups * channels) + d_skip * inputs.astype(jnp.float32)
    return jax.nn.gelu(skipped).astype(jnp.bfloat16)

def reference(mix_in, mix_gain, lam_re, lam_im, log_dt, b_re, b_im, c_re, c_im, d_skip, log_retain, w_lin, w_glu, moe_in, moe_gain, routes, route_weight, w_gate, w_up, w_down):
    normed = root_mean_normed(mix_in, mix_gain)
    log_mag, angle, drive_re, drive_im = discretize(lam_re, lam_im, log_dt, b_re, b_im)
    block_inputs = normed.reshape(TOKA // TA_DEV, TA_DEV, D)
    block_retain = log_retain.reshape(TOKA // TA_DEV, TA_DEV, GROUPS)

    def advance(carry, pieces):
        carry_re, carry_im = carry
        inputs, retain = pieces
        pref_re, pref_im, local_re, local_im = local_scan(inputs, retain, log_mag, angle, drive_re, drive_im)
        total_re = local_re + pref_re * carry_re - pref_im * carry_im
        total_im = local_im + pref_re * carry_im + pref_im * carry_re
        return ((total_re[-1], total_im[-1]), read_out(total_re, total_im, inputs, c_re, c_im, d_skip))
    anchor = jnp.zeros((GROUPS * STATE,), jnp.float32)
    _, blocks_out = lax.scan(advance, (anchor, anchor), (block_inputs, block_retain))
    activated = blocks_out.reshape(TOKA, D)
    mix_lin = jnp.dot(activated, w_lin, preferred_element_type=jnp.float32)
    mix_glu = jnp.dot(activated, w_glu, preferred_element_type=jnp.float32)
    mix_out = (mix_lin * jax.nn.sigmoid(mix_glu)).astype(jnp.bfloat16)
    normed_b = root_mean_normed(moe_in, moe_gain)
    flat_routes = routes.reshape(-1)
    assigns = flat_routes.shape[0]
    padded = jnp.concatenate([normed_b, jnp.zeros((1, D), jnp.bfloat16)], axis=0)

    def expert_rows(table, expert):
        picks = jnp.nonzero(flat_routes == expert, size=CAP * N_EP, fill_value=assigns)[0].astype(jnp.int32)
        chosen = padded[picks // TOP]
        gate_pre = jnp.dot(chosen, w_gate[expert], preferred_element_type=jnp.float32)
        up_pre = jnp.dot(chosen, w_up[expert], preferred_element_type=jnp.float32)
        hidden = (jax.nn.silu(gate_pre) * up_pre).astype(jnp.bfloat16)
        blocked = hidden.reshape(-1, N_TP, H // N_TP).astype(jnp.float32)
        down_blocks = w_down[expert].reshape(N_TP, H // N_TP, D).astype(jnp.float32)
        partials = jnp.einsum('rkh,khd->rkd', blocked, down_blocks).astype(jnp.bfloat16)
        partials = lax.optimization_barrier(partials)
        result = lax.optimization_barrier(jnp.sum(partials.astype(jnp.float32), axis=1)).astype(jnp.bfloat16)
        return (table.at[picks].set(result), None)
    opening_lookup = jnp.zeros((assigns + 1, D), jnp.bfloat16)
    table, _ = lax.scan(expert_rows, opening_lookup, jnp.arange(EXPERTS, dtype=jnp.int32))
    gathered = table[:assigns].reshape(TOKB, TOP, D).astype(jnp.float32)
    moe_out = lax.optimization_barrier(jnp.sum(gathered * route_weight[:, :, None], axis=1)).astype(jnp.bfloat16)
    return (mix_out, moe_out)
```

```python
import functools

import jax
import jax.numpy as jnp
from jax import lax
from jax.experimental import pallas as pl
from jax.experimental.pallas import tpu as pltpu
from jax.sharding import PartitionSpec as P

EPS = 1e-06


def root_mean_normed(values, gain):
    broadened_rows = values.astype(jnp.float32)
    inverse = lax.rsqrt(jnp.mean(broadened_rows * broadened_rows, axis=-1, keepdims=True) + EPS)
    return (broadened_rows * inverse * gain).astype(jnp.bfloat16)


def discretize(lam_re, lam_im, log_dt):
    time_step = jnp.exp(log_dt)[:, None]
    log_mag = lam_re * time_step
    angle = lam_im * time_step
    half_sine = jnp.sin(0.5 * angle)
    minus_re = jnp.expm1(log_mag) * jnp.cos(angle) - 2.0 * half_sine * half_sine
    minus_im = jnp.exp(log_mag) * jnp.sin(angle)
    denom = lam_re * lam_re + lam_im * lam_im
    coef_re = (minus_re * lam_re + minus_im * lam_im) / denom
    coef_im = (minus_im * lam_re - minus_re * lam_im) / denom
    magnitude = jnp.exp(log_mag)
    return coef_re, coef_im, magnitude * jnp.cos(angle), magnitude * jnp.sin(angle)


CHUNKS = 8
LANES = 128
MESH = pl.DeviceIdType.MESH


def split(value, terms):
    parts = []
    for _ in range(terms):
        part = value.astype(jnp.bfloat16)
        parts.append(part)
        value = value - part.astype(jnp.float32)
    return parts


def cmul(a_re, a_im, b_re, b_im):
    return a_re * b_re - a_im * b_im, a_re * b_im + a_im * b_re


def cpow(re, im, power):
    out = None
    while power:
        if power & 1:
            out = (re, im) if out is None else cmul(*out, re, im)
        power >>= 1
        if power:
            re, im = cmul(re, im, re, im)
    return out


def mixer_kernel(
    n_ep, n_tp, sizes, u_ref, keep_ref, coef_ref, mats_ref, skip_ref, out_ref,
    mag, push_re, push_im, ends, first, packed, gath, send_sem, recv_sem, tp_send, tp_recv,
):
    length, groups, states, channels = sizes
    width = groups * states
    steps = length // CHUNKS
    span_groups = LANES // channels
    span = span_groups * states
    spans = groups // span_groups
    rows = width // LANES
    per_span = span // LANES
    me, mine = lax.axis_index("ep"), lax.axis_index("tp")

    barrier = pltpu.get_barrier_semaphore()
    for d in range(1, n_ep):
        pl.semaphore_signal(
            barrier, inc=1, device_id=(lax.rem(me + d, n_ep), mine), device_id_type=MESH
        )
    for d in range(1, n_tp):
        pl.semaphore_signal(
            barrier, inc=1, device_id=(me, lax.rem(mine + d, n_tp)), device_id_type=MESH
        )

    def dot(x, y, dims=((1,), (0,))):
        return lax.dot_general(x, y, (dims, ((), ())), preferred_element_type=jnp.float32)

    row = lax.broadcasted_iota(jnp.int32, (length, length), 0)
    col = lax.broadcasted_iota(jnp.int32, (length, length), 1)
    order = ((row & (CHUNKS - 1)) * steps + (row >> 3) == col).astype(jnp.bfloat16)
    back = ((col & (CHUNKS - 1)) * steps + (col >> 3) == row).astype(jnp.bfloat16)
    u = dot(order, u_ref[...]).astype(jnp.bfloat16)
    keeps = [
        dot(order, part).astype(jnp.bfloat16) for part in split(jnp.exp(keep_ref[...]), 3)
    ]
    row = lax.broadcasted_iota(jnp.int32, (LANES, span), 0)
    col = lax.broadcasted_iota(jnp.int32, (LANES, span), 1)
    same = jnp.zeros((LANES, span), jnp.bool_)
    for g in range(span_groups):
        same = same | (
            (row >= g * channels) & (row < (g + 1) * channels)
            & (col >= g * states) & (col < (g + 1) * states)
        )

    def spread(value):
        return jnp.where(same, jnp.concatenate([value] * span_groups, axis=0), 0.0)

    for s in range(spans):
        at = slice(s * span, (s + 1) * span)
        group = lax.broadcasted_iota(jnp.int32, (groups, span), 0)
        lane = lax.broadcasted_iota(jnp.int32, (groups, span), 1) + s * span
        chosen = ((lane >= group * states) & (lane < (group + 1) * states)).astype(jnp.bfloat16)
        mag[:, at] = sum(dot(part, chosen) for part in keeps)
        b_re, b_im = mats_ref[0, :, at], mats_ref[1, :, at]
        co_re, co_im = coef_ref[0:1, at], coef_ref[1:2, at]
        own = u[:, s * LANES : (s + 1) * LANES]
        drive_re, drive_im = cmul(co_re, co_im, b_re, b_im)
        push_re[:, at] = sum(dot(own, part) for part in split(spread(drive_re), 2))
        push_im[:, at] = sum(dot(own, part) for part in split(spread(drive_im), 2))

    for s in range(spans):
        at = slice(s * span, (s + 1) * span)
        w_re = jnp.broadcast_to(coef_ref[2:3, at], (CHUNKS, span))
        w_im = jnp.broadcast_to(coef_ref[3:4, at], (CHUNKS, span))

        def turn(j, state, at=at, w_re=w_re, w_im=w_im):
            re, im, total = state
            here = pl.ds(pl.multiple_of(j * CHUNKS, CHUNKS), CHUNKS)
            m = mag[here, at]
            d_re, d_im = m * w_re, m * w_im
            re, im = cmul(d_re, d_im, re, im)
            return re + push_re[here, at], im + push_im[here, at], total * m

        zero = jnp.zeros((CHUNKS, span), jnp.float32)
        re, im, total = lax.fori_loop(0, steps, turn, (zero, zero, zero + 1.0))
        p_re, p_im = cpow(w_re, w_im, steps)
        ends[0, :, at] = re
        ends[1, :, at] = im
        ends[2, :, at] = total * p_re
        ends[3, :, at] = total * p_im
        ends[4, :, at] = total

    def chain(s, re, im, keep_all):
        at = slice(s * span, (s + 1) * span)
        for k in range(CHUNKS):
            if keep_all:
                first[0, k : k + 1, at] = re
                first[1, k : k + 1, at] = im
            if k < CHUNKS - 1 or not keep_all:
                re, im = cmul(ends[2, k : k + 1, at], ends[3, k : k + 1, at], re, im)
                re = re + ends[0, k : k + 1, at]
                im = im + ends[1, k : k + 1, at]
        return re, im

    for s in range(spans):
        at = slice(s * span, (s + 1) * span)
        zero = jnp.zeros((1, span), jnp.float32)
        re, im = chain(s, zero, zero, False)
        total = ends[4, 0:1, at]
        for k in range(1, CHUNKS):
            total = total * ends[4, k : k + 1, at]
        w_re, w_im = cpow(coef_ref[2:3, at], coef_ref[3:4, at], length)
        for i in range(per_span):
            r, cut = s * per_span + i, slice(i * LANES, (i + 1) * LANES)
            gath[me, r : r + 1, :] = re[:, cut]
            gath[me, rows + r : rows + r + 1, :] = im[:, cut]
            gath[me, 2 * rows + r : 2 * rows + r + 1, :] = total[:, cut]
            packed[r : r + 1, :] = w_re[:, cut]
            packed[rows + r : rows + r + 1, :] = w_im[:, cut]

    pl.semaphore_wait(barrier, n_ep - 1 + n_tp - 1)
    copies = []
    for d in range(1, n_ep):
        copy = pltpu.make_async_remote_copy(
            src_ref=gath.at[me], dst_ref=gath.at[me],
            send_sem=send_sem.at[d - 1], recv_sem=recv_sem.at[d - 1],
            device_id=(lax.rem(me + d, n_ep), mine), device_id_type=MESH,
        )
        copy.start()
        copies.append(copy)
    for copy in copies:
        copy.wait()
    wl_re, wl_im = packed[0:rows, :], packed[rows : 2 * rows, :]

    def join(i, state):
        re, im = state
        total = gath[i, 2 * rows : 3 * rows, :]
        n_re, n_im = cmul(total * wl_re, total * wl_im, re, im)
        n_re = n_re + gath[i, 0:rows, :]
        n_im = n_im + gath[i, rows : 2 * rows, :]
        return jnp.where(i < me, n_re, re), jnp.where(i < me, n_im, im)

    zero = jnp.zeros((rows, LANES), jnp.float32)
    in_re, in_im = lax.fori_loop(0, n_ep - 1, join, (zero, zero))
    packed[0:rows, :] = in_re
    packed[rows : 2 * rows, :] = in_im

    for s in range(spans):
        at = slice(s * span, (s + 1) * span)
        lines = range(s * per_span, (s + 1) * per_span)
        re = jnp.concatenate([packed[r : r + 1, :] for r in lines], axis=1)
        im = jnp.concatenate([packed[rows + r : rows + r + 1, :] for r in lines], axis=1)
        chain(s, re, im, True)
        w_re = jnp.broadcast_to(coef_ref[2:3, at], (CHUNKS, span))
        w_im = jnp.broadcast_to(coef_ref[3:4, at], (CHUNKS, span))

        def again(j, state, at=at, w_re=w_re, w_im=w_im):
            re, im = state
            here = pl.ds(pl.multiple_of(j * CHUNKS, CHUNKS), CHUNKS)
            m = mag[here, at]
            re, im = cmul(m * w_re, m * w_im, re, im)
            re, im = re + push_re[here, at], im + push_im[here, at]
            push_re[here, at] = re
            push_im[here, at] = im
            return re, im

        lax.fori_loop(0, steps, again, (first[0, :, at], first[1, :, at]))

    for s in range(spans):
        at = slice(s * span, (s + 1) * span)
        cut = slice(s * LANES, (s + 1) * LANES)
        mixed = jnp.zeros((length, LANES), jnp.float32)
        for ref, which, sign in ((push_re, 2, 1.0), (push_im, 3, -1.0)):
            x_hi, x_lo = split(ref[:, at], 2)
            c_hi, c_lo = split(spread(mats_ref[which, :, at]) * sign, 2)
            across = ((1,), (1,))
            mixed = mixed + dot(x_hi, c_hi, across)
            mixed = mixed + dot(x_hi, c_lo, across) + dot(x_lo, c_hi, across)
        x = mixed + skip_ref[:, cut] * u[:, cut].astype(jnp.float32)
        inner = 0.7978845608028654 * (x + 0.044715 * (x * x * x))
        act = (0.5 * x * (1.0 + jnp.tanh(inner))).astype(jnp.bfloat16)
        start = pl.multiple_of(mine * (spans * LANES) + s * LANES, LANES)
        out_ref[:, pl.ds(start, LANES)] = dot(back, act).astype(jnp.bfloat16)

    block = pl.ds(pl.multiple_of(mine * (spans * LANES), LANES), spans * LANES)
    copies = []
    for d in range(1, n_tp):
        copy = pltpu.make_async_remote_copy(
            src_ref=out_ref.at[:, block], dst_ref=out_ref.at[:, block],
            send_sem=tp_send.at[d - 1], recv_sem=tp_recv.at[d - 1],
            device_id=(me, lax.rem(mine + d, n_tp)), device_id_type=MESH,
        )
        copy.start()
        copies.append(copy)
    for copy in copies:
        copy.wait()


def mixer(inputs, retain, lam_re, lam_im, log_dt, b_re, b_im, c_re, c_im, d_skip):
    length, here = inputs.shape
    groups, channels, states = c_re.shape
    width = groups * states
    n_ep, n_tp = lax.axis_size("ep"), lax.axis_size("tp")
    coef = jnp.stack(discretize(lam_re, lam_im, log_dt)).reshape(4, width)
    mats = jnp.stack(
        [
            jnp.transpose(b_re, (2, 0, 1)),
            jnp.transpose(b_im, (2, 0, 1)),
            jnp.transpose(c_re, (1, 0, 2)),
            jnp.transpose(c_im, (1, 0, 2)),
        ]
    ).reshape(4, channels, width)
    rows = width // LANES
    big = pltpu.VMEM((length, width), jnp.float32)
    dma = pltpu.SemaphoreType.DMA
    return pl.pallas_call(
        functools.partial(mixer_kernel, n_ep, n_tp, (length, groups, states, channels)),
        out_shape=jax.ShapeDtypeStruct((length, here * n_tp), jnp.bfloat16),
        in_specs=[pl.BlockSpec(memory_space=pltpu.VMEM)] * 5,
        out_specs=pl.BlockSpec(memory_space=pltpu.VMEM),
        scratch_shapes=[
            big, big, big,
            pltpu.VMEM((5, CHUNKS, width), jnp.float32),
            pltpu.VMEM((2, CHUNKS, width), jnp.float32),
            pltpu.VMEM((2 * rows, LANES), jnp.float32),
            pltpu.VMEM((n_ep, 3 * rows, LANES), jnp.float32),
            dma((n_ep - 1,)), dma((n_ep - 1,)), dma((n_tp - 1,)), dma((n_tp - 1,)),
        ],
        compiler_params=pltpu.CompilerParams(collective_id=0, has_side_effects=True),
        cost_estimate=pl.CostEstimate(
            flops=20_000_000_000, bytes_accessed=4_000_000, transcendentals=0
        ),
    )(inputs, retain, coef, mats, d_skip.reshape(1, here))


def local(
    mix_in,
    mix_gain,
    lam_re,
    lam_im,
    log_dt,
    b_re,
    b_im,
    c_re,
    c_im,
    d_skip,
    log_retain,
    w_lin,
    w_glu,
    moe_in,
    moe_gain,
    routes,
    route_weight,
    w_gate,
    w_up,
    w_down,
):
    normed = root_mean_normed(mix_in, mix_gain)
    channels_here = d_skip.shape[0]
    own_inputs = lax.dynamic_slice_in_dim(
        normed, lax.axis_index("tp") * channels_here, channels_here, 1
    )
    piece = mixer(
        own_inputs, log_retain, lam_re, lam_im, log_dt, b_re, b_im, c_re, c_im, d_skip
    )
    mix_lin = jnp.dot(piece, w_lin, preferred_element_type=jnp.float32)
    mix_glu = jnp.dot(piece, w_glu, preferred_element_type=jnp.float32)
    mix_out = (mix_lin * jax.nn.sigmoid(mix_glu)).astype(jnp.bfloat16)
    normed_b = root_mean_normed(moe_in, moe_gain)
    experts = lax.axis_size("ep")
    tokens_here, choices_each = routes.shape
    capacity = 3 * choices_each * tokens_here // (2 * experts)
    flat_routes = routes.reshape(-1)
    onehot = (flat_routes[:, None] == jnp.arange(experts, dtype=jnp.int32)[None, :]).astype(
        jnp.int32
    )
    earlier_count = jnp.cumsum(onehot, axis=0) - onehot
    slot_index = jnp.sum(earlier_count * onehot, axis=1)
    target = flat_routes * capacity + slot_index
    places = jnp.arange(experts * capacity, dtype=jnp.int32)
    picked = jnp.any(
        places[:, None, None] == target.reshape(tokens_here, choices_each)[None], axis=2
    )
    picked = picked.astype(jnp.bfloat16)
    feature_slice = moe_in.shape[1] // lax.axis_size("tp")
    source_rows = lax.dynamic_slice_in_dim(
        normed_b, lax.axis_index("tp") * feature_slice, feature_slice, 1
    )
    outgoing = jnp.dot(picked, source_rows, preferred_element_type=jnp.float32).astype(jnp.bfloat16)
    outgoing = outgoing.reshape(experts, capacity, source_rows.shape[1])
    gate_local = w_gate[0]
    up_local = w_up[0]
    down_local = w_down[0]
    received = lax.all_to_all(outgoing, "ep", split_axis=0, concat_axis=0, tiled=True)
    senders, slots_here, features_here = received.shape
    piece = lax.all_gather(received, "tp", axis=2, tiled=True)
    piece_rows = piece.reshape(senders * slots_here, piece.shape[2])
    gate_pre = jnp.dot(piece_rows, gate_local, preferred_element_type=jnp.float32)
    up_pre = jnp.dot(piece_rows, up_local, preferred_element_type=jnp.float32)
    hidden = (jax.nn.silu(gate_pre) * up_pre).astype(jnp.bfloat16)
    partial_out = jnp.dot(hidden, down_local, preferred_element_type=jnp.float32).astype(
        jnp.bfloat16
    )
    partial_out = lax.optimization_barrier(partial_out)
    summed = lax.psum_scatter(
        partial_out.astype(jnp.float32).astype(jnp.bfloat16), "tp", scatter_dimension=1, tiled=True
    ).astype(jnp.float32)
    final_result = summed.astype(jnp.bfloat16).reshape(senders, slots_here, summed.shape[1])
    returned = lax.all_to_all(final_result, "ep", split_axis=0, concat_axis=0, tiled=True)
    flat_returned = returned.reshape(experts * capacity, returned.shape[2])
    gathered = (
        flat_returned[target]
        .astype(jnp.float32)
        .reshape(tokens_here, choices_each, returned.shape[2])
    )
    moe_out = jnp.sum(gathered * route_weight[:, :, None], axis=1).astype(jnp.bfloat16)
    return (mix_out, moe_out)


def solution(mesh):
    placed = (
        P("ep", None),
        P(),
        P("tp", None),
        P("tp", None),
        P("tp"),
        P("tp", None, None),
        P("tp", None, None),
        P("tp", None, None),
        P("tp", None, None),
        P("tp"),
        P("ep", "tp"),
        P(None, "tp"),
        P(None, "tp"),
        P("ep", None),
        P(),
        P("ep", None),
        P("ep", None),
        P("ep", None, "tp"),
        P("ep", None, "tp"),
        P("ep", "tp", None),
    )
    return jax.shard_map(
        local, mesh=mesh, in_specs=placed, out_specs=(P("ep", "tp"), P("ep", "tp")), check_vma=False
    )
```

```python
import functools

import jax
import jax.numpy as jnp
from jax import lax
from jax.experimental import pallas as pl
from jax.experimental.pallas import tpu as pltpu
from jax.sharding import PartitionSpec as P

EPS = 1e-06


def root_mean_normed(values, gain):
    broadened_rows = values.astype(jnp.float32)
    inverse = lax.rsqrt(jnp.mean(broadened_rows * broadened_rows, axis=-1, keepdims=True) + EPS)
    return (broadened_rows * inverse * gain).astype(jnp.bfloat16)


def discretize(lam_re, lam_im, log_dt):
    time_step = jnp.exp(log_dt)[:, None]
    log_mag = lam_re * time_step
    angle = lam_im * time_step
    half_sine = jnp.sin(0.5 * angle)
    minus_re = jnp.expm1(log_mag) * jnp.cos(angle) - 2.0 * half_sine * half_sine
    minus_im = jnp.exp(log_mag) * jnp.sin(angle)
    denom = lam_re * lam_re + lam_im * lam_im
    coef_re = (minus_re * lam_re + minus_im * lam_im) / denom
    coef_im = (minus_im * lam_re - minus_re * lam_im) / denom
    magnitude = jnp.exp(log_mag)
    return coef_re, coef_im, magnitude * jnp.cos(angle), magnitude * jnp.sin(angle)


CHUNKS = 8
LANES = 128
MESH = pl.DeviceIdType.MESH


def split(value, terms):
    parts = []
    for _ in range(terms):
        part = value.astype(jnp.bfloat16)
        parts.append(part)
        value = value - part.astype(jnp.float32)
    return parts


def cmul(a_re, a_im, b_re, b_im):
    return a_re * b_re - a_im * b_im, a_re * b_im + a_im * b_re


def cpow(re, im, power):
    out = None
    while power:
        if power & 1:
            out = (re, im) if out is None else cmul(*out, re, im)
        power >>= 1
        if power:
            re, im = cmul(re, im, re, im)
    return out


def mixer_kernel(
    n_ep, n_tp, sizes, u_ref, keep_ref, coef_ref, mats_ref, skip_ref, rows_ref, out_ref, got_ref,
    mag, push_re, push_im, ends, first, packed, gath, send_sem, recv_sem, tp_send, tp_recv,
    route_send, route_recv, share_send, share_recv,
):
    length, groups, states, channels = sizes
    width = groups * states
    steps = length // CHUNKS
    span_groups = LANES // channels
    span = span_groups * states
    spans = groups // span_groups
    rows = width // LANES
    per_span = span // LANES
    me, mine = lax.axis_index("ep"), lax.axis_index("tp")

    barrier = pltpu.get_barrier_semaphore()
    for d in range(1, n_ep):
        pl.semaphore_signal(
            barrier, inc=1, device_id=(lax.rem(me + d, n_ep), mine), device_id_type=MESH
        )
    for d in range(1, n_tp):
        pl.semaphore_signal(
            barrier, inc=1, device_id=(me, lax.rem(mine + d, n_tp)), device_id_type=MESH
        )

    features = rows_ref.shape[2]
    columns = pl.ds(pl.multiple_of(mine * features, LANES), features)

    def route(d):
        return pltpu.make_async_remote_copy(
            src_ref=rows_ref.at[lax.rem(me + d, n_ep)], dst_ref=got_ref.at[me, :, columns],
            send_sem=route_send.at[d - 1], recv_sem=route_recv.at[d - 1],
            device_id=(lax.rem(me + d, n_ep), mine), device_id_type=MESH,
        )

    def share(d, hop, source=None):
        sender = lax.rem(me + n_ep - d, n_ep)
        block = got_ref.at[sender, :, columns]
        return pltpu.make_async_remote_copy(
            src_ref=block if source is None else source, dst_ref=block,
            send_sem=share_send.at[d, hop - 1], recv_sem=share_recv.at[d, hop - 1],
            device_id=(me, lax.rem(mine + hop, n_tp)), device_id_type=MESH,
        )

    def forward(low, high):
        @pl.loop(low, high)
        def _(d):
            route(d).wait_recv()
            for hop in range(1, n_tp):
                share(d, hop).start()

    pl.semaphore_wait(barrier, n_ep - 1 + n_tp - 1)

    @pl.loop(1, n_ep)
    def _(d):
        route(d).start()

    for hop in range(1, n_tp):
        share(0, hop, rows_ref.at[me]).start()
    got_ref[me, :, columns] = rows_ref[me]

    def dot(x, y, dims=((1,), (0,))):
        return lax.dot_general(x, y, (dims, ((), ())), preferred_element_type=jnp.float32)

    row = lax.broadcasted_iota(jnp.int32, (length, length), 0)
    col = lax.broadcasted_iota(jnp.int32, (length, length), 1)
    order = ((row & (CHUNKS - 1)) * steps + (row >> 3) == col).astype(jnp.bfloat16)
    back = ((col & (CHUNKS - 1)) * steps + (col >> 3) == row).astype(jnp.bfloat16)
    u = dot(order, u_ref[...]).astype(jnp.bfloat16)
    keeps = [
        dot(order, part).astype(jnp.bfloat16) for part in split(jnp.exp(keep_ref[...]), 3)
    ]
    row = lax.broadcasted_iota(jnp.int32, (LANES, span), 0)
    col = lax.broadcasted_iota(jnp.int32, (LANES, span), 1)
    same = jnp.zeros((LANES, span), jnp.bool_)
    for g in range(span_groups):
        same = same | (
            (row >= g * channels) & (row < (g + 1) * channels)
            & (col >= g * states) & (col < (g + 1) * states)
        )

    def spread(value):
        return jnp.where(same, jnp.concatenate([value] * span_groups, axis=0), 0.0)

    for s in range(spans):
        at = slice(s * span, (s + 1) * span)
        group = lax.broadcasted_iota(jnp.int32, (groups, span), 0)
        lane = lax.broadcasted_iota(jnp.int32, (groups, span), 1) + s * span
        chosen = ((lane >= group * states) & (lane < (group + 1) * states)).astype(jnp.bfloat16)
        mag[:, at] = sum(dot(part, chosen) for part in keeps)
        b_re, b_im = mats_ref[0, :, at], mats_ref[1, :, at]
        co_re, co_im = coef_ref[0:1, at], coef_ref[1:2, at]
        own = u[:, s * LANES : (s + 1) * LANES]
        drive_re, drive_im = cmul(co_re, co_im, b_re, b_im)
        push_re[:, at] = sum(dot(own, part) for part in split(spread(drive_re), 2))
        push_im[:, at] = sum(dot(own, part) for part in split(spread(drive_im), 2))
        forward(1 + (n_ep - 1) * s // (2 * spans), 1 + (n_ep - 1) * (s + 1) // (2 * spans))

    for s in range(spans):
        at = slice(s * span, (s + 1) * span)
        w_re = jnp.broadcast_to(coef_ref[2:3, at], (CHUNKS, span))
        w_im = jnp.broadcast_to(coef_ref[3:4, at], (CHUNKS, span))

        def turn(j, state, at=at, w_re=w_re, w_im=w_im):
            re, im, total = state
            here = pl.ds(pl.multiple_of(j * CHUNKS, CHUNKS), CHUNKS)
            m = mag[here, at]
            d_re, d_im = m * w_re, m * w_im
            re, im = cmul(d_re, d_im, re, im)
            return re + push_re[here, at], im + push_im[here, at], total * m

        zero = jnp.zeros((CHUNKS, span), jnp.float32)
        re, im, total = lax.fori_loop(0, steps, turn, (zero, zero, zero + 1.0))
        p_re, p_im = cpow(w_re, w_im, steps)
        ends[0, :, at] = re
        ends[1, :, at] = im
        ends[2, :, at] = total * p_re
        ends[3, :, at] = total * p_im
        ends[4, :, at] = total

    def chain(s, re, im, keep_all):
        at = slice(s * span, (s + 1) * span)
        for k in range(CHUNKS):
            if keep_all:
                first[0, k : k + 1, at] = re
                first[1, k : k + 1, at] = im
            if k < CHUNKS - 1 or not keep_all:
                re, im = cmul(ends[2, k : k + 1, at], ends[3, k : k + 1, at], re, im)
                re = re + ends[0, k : k + 1, at]
                im = im + ends[1, k : k + 1, at]
        return re, im

    for s in range(spans):
        at = slice(s * span, (s + 1) * span)
        zero = jnp.zeros((1, span), jnp.float32)
        re, im = chain(s, zero, zero, False)
        total = ends[4, 0:1, at]
        for k in range(1, CHUNKS):
            total = total * ends[4, k : k + 1, at]
        w_re, w_im = cpow(coef_ref[2:3, at], coef_ref[3:4, at], length)
        for i in range(per_span):
            r, cut = s * per_span + i, slice(i * LANES, (i + 1) * LANES)
            gath[me, r : r + 1, :] = re[:, cut]
            gath[me, rows + r : rows + r + 1, :] = im[:, cut]
            gath[me, 2 * rows + r : 2 * rows + r + 1, :] = total[:, cut]
            packed[r : r + 1, :] = w_re[:, cut]
            packed[rows + r : rows + r + 1, :] = w_im[:, cut]

    copies = []
    for d in range(1, n_ep):
        copy = pltpu.make_async_remote_copy(
            src_ref=gath.at[me], dst_ref=gath.at[me],
            send_sem=send_sem.at[d - 1], recv_sem=recv_sem.at[d - 1],
            device_id=(lax.rem(me + d, n_ep), mine), device_id_type=MESH,
        )
        copy.start()
        copies.append(copy)
    forward(1 + (n_ep - 1) // 2, n_ep)
    for copy in copies:
        copy.wait()
    wl_re, wl_im = packed[0:rows, :], packed[rows : 2 * rows, :]

    def join(i, state):
        re, im = state
        total = gath[i, 2 * rows : 3 * rows, :]
        n_re, n_im = cmul(total * wl_re, total * wl_im, re, im)
        n_re = n_re + gath[i, 0:rows, :]
        n_im = n_im + gath[i, rows : 2 * rows, :]
        return jnp.where(i < me, n_re, re), jnp.where(i < me, n_im, im)

    zero = jnp.zeros((rows, LANES), jnp.float32)
    in_re, in_im = lax.fori_loop(0, n_ep - 1, join, (zero, zero))
    packed[0:rows, :] = in_re
    packed[rows : 2 * rows, :] = in_im

    for s in range(spans):
        at = slice(s * span, (s + 1) * span)
        lines = range(s * per_span, (s + 1) * per_span)
        re = jnp.concatenate([packed[r : r + 1, :] for r in lines], axis=1)
        im = jnp.concatenate([packed[rows + r : rows + r + 1, :] for r in lines], axis=1)
        chain(s, re, im, True)
        w_re = jnp.broadcast_to(coef_ref[2:3, at], (CHUNKS, span))
        w_im = jnp.broadcast_to(coef_ref[3:4, at], (CHUNKS, span))

        def again(j, state, at=at, w_re=w_re, w_im=w_im):
            re, im = state
            here = pl.ds(pl.multiple_of(j * CHUNKS, CHUNKS), CHUNKS)
            m = mag[here, at]
            re, im = cmul(m * w_re, m * w_im, re, im)
            re, im = re + push_re[here, at], im + push_im[here, at]
            push_re[here, at] = re
            push_im[here, at] = im
            return re, im

        lax.fori_loop(0, steps, again, (first[0, :, at], first[1, :, at]))

    for s in range(spans):
        at = slice(s * span, (s + 1) * span)
        cut = slice(s * LANES, (s + 1) * LANES)
        mixed = jnp.zeros((length, LANES), jnp.float32)
        for ref, which, sign in ((push_re, 2, 1.0), (push_im, 3, -1.0)):
            x_hi, x_lo = split(ref[:, at], 2)
            c_hi, c_lo = split(spread(mats_ref[which, :, at]) * sign, 2)
            across = ((1,), (1,))
            mixed = mixed + dot(x_hi, c_hi, across)
            mixed = mixed + dot(x_hi, c_lo, across) + dot(x_lo, c_hi, across)
        x = mixed + skip_ref[:, cut] * u[:, cut].astype(jnp.float32)
        inner = 0.7978845608028654 * (x + 0.044715 * (x * x * x))
        act = (0.5 * x * (1.0 + jnp.tanh(inner))).astype(jnp.bfloat16)
        start = pl.multiple_of(mine * (spans * LANES) + s * LANES, LANES)
        out_ref[:, pl.ds(start, LANES)] = dot(back, act).astype(jnp.bfloat16)

    block = pl.ds(pl.multiple_of(mine * (spans * LANES), LANES), spans * LANES)
    copies = []
    for d in range(1, n_tp):
        copy = pltpu.make_async_remote_copy(
            src_ref=out_ref.at[:, block], dst_ref=out_ref.at[:, block],
            send_sem=tp_send.at[d - 1], recv_sem=tp_recv.at[d - 1],
            device_id=(me, lax.rem(mine + d, n_tp)), device_id_type=MESH,
        )
        copy.start()
        copies.append(copy)
    for copy in copies:
        copy.wait()
    for hop in range(1, n_tp):
        share(0, hop, rows_ref.at[me]).wait()

    @pl.loop(1, n_ep)
    def _(d):
        route(d).wait_send()
        for hop in range(1, n_tp):
            share(d, hop).wait()


def return_kernel(n_ep, n_tp, part_ref, out_ref, parts, summed, tp_send, tp_recv, send, recv):
    me, mine = lax.axis_index("ep"), lax.axis_index("tp")
    features = out_ref.shape[2]
    barrier = pltpu.get_barrier_semaphore()
    for d in range(1, n_ep):
        pl.semaphore_signal(
            barrier, inc=1, device_id=(lax.rem(me + d, n_ep), mine), device_id_type=MESH
        )
    for d in range(1, n_tp):
        pl.semaphore_signal(
            barrier, inc=1, device_id=(me, lax.rem(mine + d, n_tp)), device_id_type=MESH
        )
    pl.semaphore_wait(barrier, n_ep - 1 + n_tp - 1)

    def columns(index):
        return pl.ds(pl.multiple_of(index * features, LANES), features)

    def scatter(d, hop):
        owner, peer = lax.rem(me + d, n_ep), lax.rem(mine + hop, n_tp)
        return pltpu.make_async_remote_copy(
            src_ref=part_ref.at[owner, :, columns(peer)], dst_ref=parts.at[owner, hop - 1],
            send_sem=tp_send.at[d - 1, hop - 1], recv_sem=tp_recv.at[d - 1, hop - 1],
            device_id=(me, peer), device_id_type=MESH,
        )

    def home(d):
        owner = lax.rem(me + d, n_ep)
        return pltpu.make_async_remote_copy(
            src_ref=summed.at[owner], dst_ref=out_ref.at[me],
            send_sem=send.at[d - 1], recv_sem=recv.at[d - 1],
            device_id=(owner, mine), device_id_type=MESH,
        )

    def total(d):
        owner = lax.rem(me + d, n_ep)
        value = part_ref[owner, :, columns(mine)].astype(jnp.float32)
        for hop in range(1, n_tp):
            scatter(d, hop).wait_recv()
            value = value + parts[owner, hop - 1].astype(jnp.float32)
        return owner, value.astype(jnp.bfloat16)

    @pl.loop(1, n_ep + 1)
    def _(d):
        for hop in range(1, n_tp):
            scatter(d, hop).start()

    @pl.loop(1, n_ep)
    def _(d):
        owner, value = total(d)
        summed[owner] = value
        home(d).start()

    _, value = total(n_ep)
    out_ref[me] = value

    @pl.loop(1, n_ep)
    def _(d):
        home(d).wait()

    @pl.loop(1, n_ep + 1)
    def _(d):
        for hop in range(1, n_tp):
            scatter(d, hop).wait_send()


def give_back(partial_out):
    n_ep, n_tp = lax.axis_size("ep"), lax.axis_size("tp")
    _, slots, width = partial_out.shape
    features = width // n_tp
    dma = pltpu.SemaphoreType.DMA
    return pl.pallas_call(
        functools.partial(return_kernel, n_ep, n_tp),
        out_shape=jax.ShapeDtypeStruct((n_ep, slots, features), jnp.bfloat16),
        in_specs=[pl.BlockSpec(memory_space=pltpu.VMEM)],
        out_specs=pl.BlockSpec(memory_space=pltpu.VMEM),
        scratch_shapes=[
            pltpu.VMEM((n_ep, n_tp - 1, slots, features), jnp.bfloat16),
            pltpu.VMEM((n_ep, slots, features), jnp.bfloat16),
            dma((n_ep, n_tp - 1)), dma((n_ep, n_tp - 1)), dma((n_ep - 1,)), dma((n_ep - 1,)),
        ],
        compiler_params=pltpu.CompilerParams(collective_id=1, has_side_effects=True),
        cost_estimate=pl.CostEstimate(
            flops=20_000_000_000, bytes_accessed=4_000_000, transcendentals=0
        ),
    )(partial_out)


def mixer(inputs, retain, lam_re, lam_im, log_dt, b_re, b_im, c_re, c_im, d_skip, outgoing):
    length, here = inputs.shape
    groups, channels, states = c_re.shape
    width = groups * states
    n_ep, n_tp = lax.axis_size("ep"), lax.axis_size("tp")
    coef = jnp.stack(discretize(lam_re, lam_im, log_dt)).reshape(4, width)
    mats = jnp.stack(
        [
            jnp.transpose(b_re, (2, 0, 1)),
            jnp.transpose(b_im, (2, 0, 1)),
            jnp.transpose(c_re, (1, 0, 2)),
            jnp.transpose(c_im, (1, 0, 2)),
        ]
    ).reshape(4, channels, width)
    rows = width // LANES
    _, slots, features = outgoing.shape
    big = pltpu.VMEM((length, width), jnp.float32)
    dma = pltpu.SemaphoreType.DMA
    return pl.pallas_call(
        functools.partial(mixer_kernel, n_ep, n_tp, (length, groups, states, channels)),
        out_shape=(
            jax.ShapeDtypeStruct((length, here * n_tp), jnp.bfloat16),
            jax.ShapeDtypeStruct((n_ep, slots, features * n_tp), jnp.bfloat16),
        ),
        in_specs=[pl.BlockSpec(memory_space=pltpu.VMEM)] * 6,
        out_specs=(pl.BlockSpec(memory_space=pltpu.VMEM),) * 2,
        scratch_shapes=[
            big, big, big,
            pltpu.VMEM((5, CHUNKS, width), jnp.float32),
            pltpu.VMEM((2, CHUNKS, width), jnp.float32),
            pltpu.VMEM((2 * rows, LANES), jnp.float32),
            pltpu.VMEM((n_ep, 3 * rows, LANES), jnp.float32),
            dma((n_ep - 1,)), dma((n_ep - 1,)), dma((n_tp - 1,)), dma((n_tp - 1,)),
            dma((n_ep - 1,)), dma((n_ep - 1,)), dma((n_ep, n_tp - 1)), dma((n_ep, n_tp - 1)),
        ],
        compiler_params=pltpu.CompilerParams(collective_id=0, has_side_effects=True),
        cost_estimate=pl.CostEstimate(
            flops=20_000_000_000, bytes_accessed=4_000_000, transcendentals=0
        ),
    )(inputs, retain, coef, mats, d_skip.reshape(1, here), outgoing)


def local(
    mix_in,
    mix_gain,
    lam_re,
    lam_im,
    log_dt,
    b_re,
    b_im,
    c_re,
    c_im,
    d_skip,
    log_retain,
    w_lin,
    w_glu,
    moe_in,
    moe_gain,
    routes,
    route_weight,
    w_gate,
    w_up,
    w_down,
):
    normed = root_mean_normed(mix_in, mix_gain)
    channels_here = d_skip.shape[0]
    own_inputs = lax.dynamic_slice_in_dim(
        normed, lax.axis_index("tp") * channels_here, channels_here, 1
    )
    normed_b = root_mean_normed(moe_in, moe_gain)
    experts = lax.axis_size("ep")
    tokens_here, choices_each = routes.shape
    capacity = 3 * choices_each * tokens_here // (2 * experts)
    flat_routes = routes.reshape(-1)
    onehot = (flat_routes[:, None] == jnp.arange(experts, dtype=jnp.int32)[None, :]).astype(
        jnp.int32
    )
    earlier_count = jnp.cumsum(onehot, axis=0) - onehot
    slot_index = jnp.sum(earlier_count * onehot, axis=1)
    target = flat_routes * capacity + slot_index
    places = jnp.arange(experts * capacity, dtype=jnp.int32)
    picked = jnp.any(
        places[:, None, None] == target.reshape(tokens_here, choices_each)[None], axis=2
    )
    picked = picked.astype(jnp.bfloat16)
    feature_slice = moe_in.shape[1] // lax.axis_size("tp")
    source_rows = lax.dynamic_slice_in_dim(
        normed_b, lax.axis_index("tp") * feature_slice, feature_slice, 1
    )
    outgoing = jnp.dot(picked, source_rows, preferred_element_type=jnp.float32).astype(jnp.bfloat16)
    outgoing = outgoing.reshape(experts, capacity, source_rows.shape[1])
    gate_local = w_gate[0]
    up_local = w_up[0]
    down_local = w_down[0]
    piece, received = mixer(
        own_inputs, log_retain, lam_re, lam_im, log_dt, b_re, b_im, c_re, c_im, d_skip, outgoing
    )
    piece_rows = received.reshape(experts * capacity, received.shape[2])
    gate_pre = jnp.dot(piece_rows, gate_local, preferred_element_type=jnp.float32)
    up_pre = jnp.dot(piece_rows, up_local, preferred_element_type=jnp.float32)
    hidden = (jax.nn.silu(gate_pre) * up_pre).astype(jnp.bfloat16)
    partial_out = jnp.dot(hidden, down_local, preferred_element_type=jnp.float32).astype(
        jnp.bfloat16
    )
    returned = give_back(partial_out.reshape(experts, capacity, partial_out.shape[1]))
    flat_returned = returned.reshape(experts * capacity, returned.shape[2])
    gathered = (
        flat_returned[target]
        .astype(jnp.float32)
        .reshape(tokens_here, choices_each, returned.shape[2])
    )
    moe_out = jnp.sum(gathered * route_weight[:, :, None], axis=1).astype(jnp.bfloat16)
    mix_lin = jnp.dot(piece, w_lin, preferred_element_type=jnp.float32)
    mix_glu = jnp.dot(piece, w_glu, preferred_element_type=jnp.float32)
    mix_out = (mix_lin * jax.nn.sigmoid(mix_glu)).astype(jnp.bfloat16)
    return (mix_out, moe_out)


def solution(mesh):
    placed = (
        P("ep", None),
        P(),
        P("tp", None),
        P("tp", None),
        P("tp"),
        P("tp", None, None),
        P("tp", None, None),
        P("tp", None, None),
        P("tp", None, None),
        P("tp"),
        P("ep", "tp"),
        P(None, "tp"),
        P(None, "tp"),
        P("ep", None),
        P(),
        P("ep", None),
        P("ep", None),
        P("ep", None, "tp"),
        P("ep", None, "tp"),
        P("ep", "tp", None),
    )
    return jax.shard_map(
        local, mesh=mesh, in_specs=placed, out_specs=(P("ep", "tp"), P("ep", "tp")), check_vma=False
    )
```

```python
import functools

import jax
import jax.numpy as jnp
from jax import lax
from jax.experimental import pallas as pl
from jax.experimental.pallas import tpu as pltpu
from jax.sharding import PartitionSpec as P

EPS = 1e-06


def root_mean_normed(values, gain):
    broadened_rows = values.astype(jnp.float32)
    inverse = lax.rsqrt(jnp.mean(broadened_rows * broadened_rows, axis=-1, keepdims=True) + EPS)
    return (broadened_rows * inverse * gain).astype(jnp.bfloat16)


def discretize(lam_re, lam_im, log_dt):
    time_step = jnp.exp(log_dt)[:, None]
    log_mag = lam_re * time_step
    angle = lam_im * time_step
    half_sine = jnp.sin(0.5 * angle)
    minus_re = jnp.expm1(log_mag) * jnp.cos(angle) - 2.0 * half_sine * half_sine
    minus_im = jnp.exp(log_mag) * jnp.sin(angle)
    denom = lam_re * lam_re + lam_im * lam_im
    coef_re = (minus_re * lam_re + minus_im * lam_im) / denom
    coef_im = (minus_im * lam_re - minus_re * lam_im) / denom
    magnitude = jnp.exp(log_mag)
    return coef_re, coef_im, magnitude * jnp.cos(angle), magnitude * jnp.sin(angle)


CHUNKS = 8
LANES = 128
MESH = pl.DeviceIdType.MESH


def split(value, terms):
    parts = []
    for _ in range(terms):
        part = value.astype(jnp.bfloat16)
        parts.append(part)
        value = value - part.astype(jnp.float32)
    return parts


def cmul(a_re, a_im, b_re, b_im):
    return a_re * b_re - a_im * b_im, a_re * b_im + a_im * b_re


def cpow(re, im, power):
    out = None
    while power:
        if power & 1:
            out = (re, im) if out is None else cmul(*out, re, im)
        power >>= 1
        if power:
            re, im = cmul(re, im, re, im)
    return out


def mixer_kernel(
    n_ep, n_tp, sizes, u_ref, keep_ref, coef_ref, mats_ref, skip_ref, part_ref, out_ref, home_ref,
    mag, push_re, push_im, ends, first, packed, gath, send_sem, recv_sem, tp_send, tp_recv,
    route_send, route_recv, share_send, share_recv, parts, summed,
):
    length, groups, states, channels = sizes
    width = groups * states
    steps = length // CHUNKS
    span_groups = LANES // channels
    span = span_groups * states
    spans = groups // span_groups
    rows = width // LANES
    per_span = span // LANES
    me, mine = lax.axis_index("ep"), lax.axis_index("tp")

    barrier = pltpu.get_barrier_semaphore()
    for d in range(1, n_ep):
        pl.semaphore_signal(
            barrier, inc=1, device_id=(lax.rem(me + d, n_ep), mine), device_id_type=MESH
        )
    for d in range(1, n_tp):
        pl.semaphore_signal(
            barrier, inc=1, device_id=(me, lax.rem(mine + d, n_tp)), device_id_type=MESH
        )

    features = home_ref.shape[2]
    pl.semaphore_wait(barrier, n_ep - 1 + n_tp - 1)

    def columns(index):
        return pl.ds(pl.multiple_of(index * features, LANES), features)

    def scatter(d, hop):
        owner, peer = lax.rem(me + d, n_ep), lax.rem(mine + hop, n_tp)
        return pltpu.make_async_remote_copy(
            src_ref=part_ref.at[owner, :, columns(peer)], dst_ref=parts.at[owner, hop - 1],
            send_sem=share_send.at[d - 1, hop - 1], recv_sem=share_recv.at[d - 1, hop - 1],
            device_id=(me, peer), device_id_type=MESH,
        )

    def home(d):
        owner = lax.rem(me + d, n_ep)
        return pltpu.make_async_remote_copy(
            src_ref=summed.at[owner], dst_ref=home_ref.at[me],
            send_sem=route_send.at[d - 1], recv_sem=route_recv.at[d - 1],
            device_id=(owner, mine), device_id_type=MESH,
        )

    def added(d):
        owner = lax.rem(me + d, n_ep)
        value = part_ref[owner, :, columns(mine)].astype(jnp.float32)
        for hop in range(1, n_tp):
            scatter(d, hop).wait_recv()
            value = value + parts[owner, hop - 1].astype(jnp.float32)
        return owner, value.astype(jnp.bfloat16)

    @pl.loop(1, n_ep + 1)
    def _(d):
        for hop in range(1, n_tp):
            scatter(d, hop).start()

    def forward(low, high):
        @pl.loop(low, high)
        def _(d):
            owner, value = added(d)
            summed[owner] = value
            home(d).start()

    def dot(x, y, dims=((1,), (0,))):
        return lax.dot_general(x, y, (dims, ((), ())), preferred_element_type=jnp.float32)

    row = lax.broadcasted_iota(jnp.int32, (length, length), 0)
    col = lax.broadcasted_iota(jnp.int32, (length, length), 1)
    order = ((row & (CHUNKS - 1)) * steps + (row >> 3) == col).astype(jnp.bfloat16)
    back = ((col & (CHUNKS - 1)) * steps + (col >> 3) == row).astype(jnp.bfloat16)
    u = dot(order, u_ref[...]).astype(jnp.bfloat16)
    keeps = [
        dot(order, part).astype(jnp.bfloat16) for part in split(jnp.exp(keep_ref[...]), 3)
    ]
    row = lax.broadcasted_iota(jnp.int32, (LANES, span), 0)
    col = lax.broadcasted_iota(jnp.int32, (LANES, span), 1)
    same = jnp.zeros((LANES, span), jnp.bool_)
    for g in range(span_groups):
        same = same | (
            (row >= g * channels) & (row < (g + 1) * channels)
            & (col >= g * states) & (col < (g + 1) * states)
        )

    def spread(value):
        return jnp.where(same, jnp.concatenate([value] * span_groups, axis=0), 0.0)

    for s in range(spans):
        at = slice(s * span, (s + 1) * span)
        group = lax.broadcasted_iota(jnp.int32, (groups, span), 0)
        lane = lax.broadcasted_iota(jnp.int32, (groups, span), 1) + s * span
        chosen = ((lane >= group * states) & (lane < (group + 1) * states)).astype(jnp.bfloat16)
        mag[:, at] = sum(dot(part, chosen) for part in keeps)
        b_re, b_im = mats_ref[0, :, at], mats_ref[1, :, at]
        co_re, co_im = coef_ref[0:1, at], coef_ref[1:2, at]
        own = u[:, s * LANES : (s + 1) * LANES]
        drive_re, drive_im = cmul(co_re, co_im, b_re, b_im)
        push_re[:, at] = sum(dot(own, part) for part in split(spread(drive_re), 2))
        push_im[:, at] = sum(dot(own, part) for part in split(spread(drive_im), 2))
        forward(1 + (n_ep - 1) * s // (2 * spans), 1 + (n_ep - 1) * (s + 1) // (2 * spans))

    for s in range(spans):
        at = slice(s * span, (s + 1) * span)
        w_re = jnp.broadcast_to(coef_ref[2:3, at], (CHUNKS, span))
        w_im = jnp.broadcast_to(coef_ref[3:4, at], (CHUNKS, span))

        def turn(j, state, at=at, w_re=w_re, w_im=w_im):
            re, im, total = state
            here = pl.ds(pl.multiple_of(j * CHUNKS, CHUNKS), CHUNKS)
            m = mag[here, at]
            d_re, d_im = m * w_re, m * w_im
            re, im = cmul(d_re, d_im, re, im)
            return re + push_re[here, at], im + push_im[here, at], total * m

        zero = jnp.zeros((CHUNKS, span), jnp.float32)
        re, im, total = lax.fori_loop(0, steps, turn, (zero, zero, zero + 1.0))
        p_re, p_im = cpow(w_re, w_im, steps)
        ends[0, :, at] = re
        ends[1, :, at] = im
        ends[2, :, at] = total * p_re
        ends[3, :, at] = total * p_im
        ends[4, :, at] = total

    def chain(s, re, im, keep_all):
        at = slice(s * span, (s + 1) * span)
        for k in range(CHUNKS):
            if keep_all:
                first[0, k : k + 1, at] = re
                first[1, k : k + 1, at] = im
            if k < CHUNKS - 1 or not keep_all:
                re, im = cmul(ends[2, k : k + 1, at], ends[3, k : k + 1, at], re, im)
                re = re + ends[0, k : k + 1, at]
                im = im + ends[1, k : k + 1, at]
        return re, im

    for s in range(spans):
        at = slice(s * span, (s + 1) * span)
        zero = jnp.zeros((1, span), jnp.float32)
        re, im = chain(s, zero, zero, False)
        total = ends[4, 0:1, at]
        for k in range(1, CHUNKS):
            total = total * ends[4, k : k + 1, at]
        w_re, w_im = cpow(coef_ref[2:3, at], coef_ref[3:4, at], length)
        for i in range(per_span):
            r, cut = s * per_span + i, slice(i * LANES, (i + 1) * LANES)
            gath[me, r : r + 1, :] = re[:, cut]
            gath[me, rows + r : rows + r + 1, :] = im[:, cut]
            gath[me, 2 * rows + r : 2 * rows + r + 1, :] = total[:, cut]
            packed[r : r + 1, :] = w_re[:, cut]
            packed[rows + r : rows + r + 1, :] = w_im[:, cut]

    copies = []
    for d in range(1, n_ep):
        copy = pltpu.make_async_remote_copy(
            src_ref=gath.at[me], dst_ref=gath.at[me],
            send_sem=send_sem.at[d - 1], recv_sem=recv_sem.at[d - 1],
            device_id=(lax.rem(me + d, n_ep), mine), device_id_type=MESH,
        )
        copy.start()
        copies.append(copy)
    forward(1 + (n_ep - 1) // 2, n_ep)
    for copy in copies:
        copy.wait()
    wl_re, wl_im = packed[0:rows, :], packed[rows : 2 * rows, :]

    def join(i, state):
        re, im = state
        total = gath[i, 2 * rows : 3 * rows, :]
        n_re, n_im = cmul(total * wl_re, total * wl_im, re, im)
        n_re = n_re + gath[i, 0:rows, :]
        n_im = n_im + gath[i, rows : 2 * rows, :]
        return jnp.where(i < me, n_re, re), jnp.where(i < me, n_im, im)

    zero = jnp.zeros((rows, LANES), jnp.float32)
    in_re, in_im = lax.fori_loop(0, n_ep - 1, join, (zero, zero))
    packed[0:rows, :] = in_re
    packed[rows : 2 * rows, :] = in_im

    for s in range(spans):
        at = slice(s * span, (s + 1) * span)
        lines = range(s * per_span, (s + 1) * per_span)
        re = jnp.concatenate([packed[r : r + 1, :] for r in lines], axis=1)
        im = jnp.concatenate([packed[rows + r : rows + r + 1, :] for r in lines], axis=1)
        chain(s, re, im, True)
        w_re = jnp.broadcast_to(coef_ref[2:3, at], (CHUNKS, span))
        w_im = jnp.broadcast_to(coef_ref[3:4, at], (CHUNKS, span))

        def again(j, state, at=at, w_re=w_re, w_im=w_im):
            re, im = state
            here = pl.ds(pl.multiple_of(j * CHUNKS, CHUNKS), CHUNKS)
            m = mag[here, at]
            re, im = cmul(m * w_re, m * w_im, re, im)
            re, im = re + push_re[here, at], im + push_im[here, at]
            push_re[here, at] = re
            push_im[here, at] = im
            return re, im

        lax.fori_loop(0, steps, again, (first[0, :, at], first[1, :, at]))

    for s in range(spans):
        at = slice(s * span, (s + 1) * span)
        cut = slice(s * LANES, (s + 1) * LANES)
        mixed = jnp.zeros((length, LANES), jnp.float32)
        for ref, which, sign in ((push_re, 2, 1.0), (push_im, 3, -1.0)):
            x_hi, x_lo = split(ref[:, at], 2)
            c_hi, c_lo = split(spread(mats_ref[which, :, at]) * sign, 2)
            across = ((1,), (1,))
            mixed = mixed + dot(x_hi, c_hi, across)
            mixed = mixed + dot(x_hi, c_lo, across) + dot(x_lo, c_hi, across)
        x = mixed + skip_ref[:, cut] * u[:, cut].astype(jnp.float32)
        inner = 0.7978845608028654 * (x + 0.044715 * (x * x * x))
        act = (0.5 * x * (1.0 + jnp.tanh(inner))).astype(jnp.bfloat16)
        start = pl.multiple_of(mine * (spans * LANES) + s * LANES, LANES)
        out_ref[:, pl.ds(start, LANES)] = dot(back, act).astype(jnp.bfloat16)

    block = pl.ds(pl.multiple_of(mine * (spans * LANES), LANES), spans * LANES)
    copies = []
    for d in range(1, n_tp):
        copy = pltpu.make_async_remote_copy(
            src_ref=out_ref.at[:, block], dst_ref=out_ref.at[:, block],
            send_sem=tp_send.at[d - 1], recv_sem=tp_recv.at[d - 1],
            device_id=(me, lax.rem(mine + d, n_tp)), device_id_type=MESH,
        )
        copy.start()
        copies.append(copy)
    for copy in copies:
        copy.wait()
    _, value = added(n_ep)
    home_ref[me] = value

    @pl.loop(1, n_ep)
    def _(d):
        home(d).wait()

    @pl.loop(1, n_ep + 1)
    def _(d):
        for hop in range(1, n_tp):
            scatter(d, hop).wait_send()


def dispatch_kernel(
    n_ep, n_tp, rows_ref, got_ref, route_send, route_recv, share_send, share_recv
):
    me, mine = lax.axis_index("ep"), lax.axis_index("tp")
    barrier = pltpu.get_barrier_semaphore()
    for d in range(1, n_ep):
        pl.semaphore_signal(
            barrier, inc=1, device_id=(lax.rem(me + d, n_ep), mine), device_id_type=MESH
        )
    for d in range(1, n_tp):
        pl.semaphore_signal(
            barrier, inc=1, device_id=(me, lax.rem(mine + d, n_tp)), device_id_type=MESH
        )

    features = rows_ref.shape[2]
    columns = pl.ds(pl.multiple_of(mine * features, LANES), features)

    def route(d):
        return pltpu.make_async_remote_copy(
            src_ref=rows_ref.at[lax.rem(me + d, n_ep)], dst_ref=got_ref.at[me, :, columns],
            send_sem=route_send.at[d - 1], recv_sem=route_recv.at[d - 1],
            device_id=(lax.rem(me + d, n_ep), mine), device_id_type=MESH,
        )

    def share(d, hop, source=None):
        sender = lax.rem(me + n_ep - d, n_ep)
        block = got_ref.at[sender, :, columns]
        return pltpu.make_async_remote_copy(
            src_ref=block if source is None else source, dst_ref=block,
            send_sem=share_send.at[d, hop - 1], recv_sem=share_recv.at[d, hop - 1],
            device_id=(me, lax.rem(mine + hop, n_tp)), device_id_type=MESH,
        )

    def forward(low, high):
        @pl.loop(low, high)
        def _(d):
            route(d).wait_recv()
            for hop in range(1, n_tp):
                share(d, hop).start()

    pl.semaphore_wait(barrier, n_ep - 1 + n_tp - 1)

    @pl.loop(1, n_ep)
    def _(d):
        route(d).start()

    for hop in range(1, n_tp):
        share(0, hop, rows_ref.at[me]).start()
    got_ref[me, :, columns] = rows_ref[me]
    forward(1, n_ep)
    for hop in range(1, n_tp):
        share(0, hop, rows_ref.at[me]).wait()

    @pl.loop(1, n_ep)
    def _(d):
        route(d).wait_send()
        for hop in range(1, n_tp):
            share(d, hop).wait()


def dispatch(outgoing):
    n_ep, n_tp = lax.axis_size("ep"), lax.axis_size("tp")
    _, slots, features = outgoing.shape
    dma = pltpu.SemaphoreType.DMA
    return pl.pallas_call(
        functools.partial(dispatch_kernel, n_ep, n_tp),
        out_shape=jax.ShapeDtypeStruct((n_ep, slots, features * n_tp), jnp.bfloat16),
        in_specs=[pl.BlockSpec(memory_space=pltpu.VMEM)],
        out_specs=pl.BlockSpec(memory_space=pltpu.VMEM),
        scratch_shapes=[
            dma((n_ep - 1,)), dma((n_ep - 1,)), dma((n_ep, n_tp - 1)), dma((n_ep, n_tp - 1)),
        ],
        compiler_params=pltpu.CompilerParams(collective_id=1, has_side_effects=True),
        cost_estimate=pl.CostEstimate(
            flops=20_000_000_000, bytes_accessed=4_000_000, transcendentals=0
        ),
    )(outgoing)


def mixer(inputs, retain, lam_re, lam_im, log_dt, b_re, b_im, c_re, c_im, d_skip, partial_out):
    length, here = inputs.shape
    groups, channels, states = c_re.shape
    width = groups * states
    n_ep, n_tp = lax.axis_size("ep"), lax.axis_size("tp")
    coef = jnp.stack(discretize(lam_re, lam_im, log_dt)).reshape(4, width)
    mats = jnp.stack(
        [
            jnp.transpose(b_re, (2, 0, 1)),
            jnp.transpose(b_im, (2, 0, 1)),
            jnp.transpose(c_re, (1, 0, 2)),
            jnp.transpose(c_im, (1, 0, 2)),
        ]
    ).reshape(4, channels, width)
    rows = width // LANES
    _, slots, features = partial_out.shape
    features = features // n_tp
    big = pltpu.VMEM((length, width), jnp.float32)
    dma = pltpu.SemaphoreType.DMA
    return pl.pallas_call(
        functools.partial(mixer_kernel, n_ep, n_tp, (length, groups, states, channels)),
        out_shape=(
            jax.ShapeDtypeStruct((length, here * n_tp), jnp.bfloat16),
            jax.ShapeDtypeStruct((n_ep, slots, features), jnp.bfloat16),
        ),
        in_specs=[pl.BlockSpec(memory_space=pltpu.VMEM)] * 6,
        out_specs=(pl.BlockSpec(memory_space=pltpu.VMEM),) * 2,
        scratch_shapes=[
            big, big, big,
            pltpu.VMEM((5, CHUNKS, width), jnp.float32),
            pltpu.VMEM((2, CHUNKS, width), jnp.float32),
            pltpu.VMEM((2 * rows, LANES), jnp.float32),
            pltpu.VMEM((n_ep, 3 * rows, LANES), jnp.float32),
            dma((n_ep - 1,)), dma((n_ep - 1,)), dma((n_tp - 1,)), dma((n_tp - 1,)),
            dma((n_ep - 1,)), dma((n_ep - 1,)), dma((n_ep, n_tp - 1)), dma((n_ep, n_tp - 1)),
            pltpu.VMEM((n_ep, n_tp - 1, slots, features), jnp.bfloat16),
            pltpu.VMEM((n_ep, slots, features), jnp.bfloat16),
        ],
        compiler_params=pltpu.CompilerParams(collective_id=0, has_side_effects=True),
        cost_estimate=pl.CostEstimate(
            flops=20_000_000_000, bytes_accessed=4_000_000, transcendentals=0
        ),
    )(inputs, retain, coef, mats, d_skip.reshape(1, here), partial_out)


def local(
    mix_in,
    mix_gain,
    lam_re,
    lam_im,
    log_dt,
    b_re,
    b_im,
    c_re,
    c_im,
    d_skip,
    log_retain,
    w_lin,
    w_glu,
    moe_in,
    moe_gain,
    routes,
    route_weight,
    w_gate,
    w_up,
    w_down,
):
    normed = root_mean_normed(mix_in, mix_gain)
    channels_here = d_skip.shape[0]
    own_inputs = lax.dynamic_slice_in_dim(
        normed, lax.axis_index("tp") * channels_here, channels_here, 1
    )
    normed_b = root_mean_normed(moe_in, moe_gain)
    experts = lax.axis_size("ep")
    tokens_here, choices_each = routes.shape
    capacity = 3 * choices_each * tokens_here // (2 * experts)
    flat_routes = routes.reshape(-1)
    onehot = (flat_routes[:, None] == jnp.arange(experts, dtype=jnp.int32)[None, :]).astype(
        jnp.int32
    )
    earlier_count = jnp.cumsum(onehot, axis=0) - onehot
    slot_index = jnp.sum(earlier_count * onehot, axis=1)
    target = flat_routes * capacity + slot_index
    places = jnp.arange(experts * capacity, dtype=jnp.int32)
    picked = jnp.any(
        places[:, None, None] == target.reshape(tokens_here, choices_each)[None], axis=2
    )
    picked = picked.astype(jnp.bfloat16)
    feature_slice = moe_in.shape[1] // lax.axis_size("tp")
    source_rows = lax.dynamic_slice_in_dim(
        normed_b, lax.axis_index("tp") * feature_slice, feature_slice, 1
    )
    outgoing = jnp.dot(picked, source_rows, preferred_element_type=jnp.float32).astype(jnp.bfloat16)
    outgoing = outgoing.reshape(experts, capacity, source_rows.shape[1])
    gate_local = w_gate[0]
    up_local = w_up[0]
    down_local = w_down[0]
    received = dispatch(outgoing)
    piece_rows = received.reshape(experts * capacity, received.shape[2])
    gate_pre = jnp.dot(piece_rows, gate_local, preferred_element_type=jnp.float32)
    up_pre = jnp.dot(piece_rows, up_local, preferred_element_type=jnp.float32)
    hidden = (jax.nn.silu(gate_pre) * up_pre).astype(jnp.bfloat16)
    partial_out = jnp.dot(hidden, down_local, preferred_element_type=jnp.float32).astype(
        jnp.bfloat16
    )
    piece, returned = mixer(
        own_inputs, log_retain, lam_re, lam_im, log_dt, b_re, b_im, c_re, c_im, d_skip,
        partial_out.reshape(experts, capacity, partial_out.shape[1]),
    )
    flat_returned = returned.reshape(experts * capacity, returned.shape[2])
    gathered = (
        flat_returned[target]
        .astype(jnp.float32)
        .reshape(tokens_here, choices_each, returned.shape[2])
    )
    moe_out = jnp.sum(gathered * route_weight[:, :, None], axis=1).astype(jnp.bfloat16)
    mix_lin = jnp.dot(piece, w_lin, preferred_element_type=jnp.float32)
    mix_glu = jnp.dot(piece, w_glu, preferred_element_type=jnp.float32)
    mix_out = (mix_lin * jax.nn.sigmoid(mix_glu)).astype(jnp.bfloat16)
    return (mix_out, moe_out)


def solution(mesh):
    placed = (
        P("ep", None),
        P(),
        P("tp", None),
        P("tp", None),
        P("tp"),
        P("tp", None, None),
        P("tp", None, None),
        P("tp", None, None),
        P("tp", None, None),
        P("tp"),
        P("ep", "tp"),
        P(None, "tp"),
        P(None, "tp"),
        P("ep", None),
        P(),
        P("ep", None),
        P("ep", None),
        P("ep", None, "tp"),
        P("ep", None, "tp"),
        P("ep", "tp", None),
    )
    return jax.shard_map(
        local, mesh=mesh, in_specs=placed, out_specs=(P("ep", "tp"), P("ep", "tp")), check_vma=False
    )
```
